1024 devices in a mesh: tp: 1024 (over z, y, x, core).
Axes of the slice: x: 8, y: 8, z: 8, core: 2. Of those that a mesh axis runs over, the one named last changes fastest.
Arguments:
- tokens: bfloat16 [1024, 8, 128], P('tp'), may hold values from -6 to 6
- block_norm_gain: float32 [2, 4096], replicated, may hold values from 0.1 to 1.9
- receptance_weight: bfloat16 [2, 1024, 128, 64], P(None, 'tp'), may hold values from -0.09375 to 0.09375
- key_weight: bfloat16 [2, 1024, 128, 64], P(None, 'tp'), may hold values from -0.09375 to 0.09375
- value_weight: bfloat16 [2, 1024, 128, 64], P(None, 'tp'), may hold values from -0.09375 to 0.09375
- decay_weight: bfloat16 [2, 1024, 128, 64], P(None, 'tp'), may hold values from -0.09375 to 0.09375
- learning_rate_weight: bfloat16 [2, 1024, 128, 64], P(None, 'tp'), may hold values from -0.09375 to 0.09375
- gate_weight: bfloat16 [2, 1024, 128, 64], P(None, 'tp'), may hold values from -0.09375 to 0.09375
- decay_bias_fixed: float32 [2, 2048], replicated, may hold values from -5 to 2
- self_token_weight: float32 [2, 2048], replicated, may hold values from -1.5 to 1.5
- readout_norm_gain: float32 [2, 2048], replicated, may hold values from 0.1 to 1.9
- output_weight: bfloat16 [2, 1024, 64, 128], P(None, 'tp'), may hold values from -0.125 to 0.125
- state: float32 [2, 1024, 8, 4096], P(None, 'tp'), may hold values from -3 to 3
Outputs:
- mixed: bfloat16 [1024, 8, 128], P('tp')
- new_state: float32 [2, 1024, 8, 4096], P(None, 'tp')
The draws below stay inside these ranges and needn't reach their ends.
All inputs are finite; a program needn't handle non-finite values.
Results may differ from the reference program's by a relative error of at most 0.018.
Values may be sent and summed in bfloat16 or wider, within the bound.
A program may use at most 32 MiB of HBM per device.

```python
import jax
import jax.numpy as jnp
from jax import lax

D = 4096
MIXER_WIDTH = 2048
HEAD_CHANNELS = 64
WINDOW_LAYERS = 2
SEQS = 256
MIXER_HEADS = 32
ROW_BLOCKS = 32
N_TP = 1024


def shard_levels(own_key, shape, split, smallest, largest):
    gain = 1.0
    for axis_at, blocks in split:
        steps = jax.random.uniform(jax.random.fold_in(jax.random.fold_in(own_key, 6), axis_at), (blocks,), jnp.float32, smallest / len(split), largest / len(split))
        gain = gain * jnp.repeat(jnp.exp(steps), shape[axis_at] // blocks).reshape((-1,) + (1,) * (len(shape) - 1 - axis_at))
    return gain


def scatter_about(own_key, shape, width, most, pieces=(), dtype=jnp.bfloat16):
    loudness = shard_levels(own_key, shape, pieces, -0.22, 0.18) if pieces else 1.0
    entries = jax.random.normal(own_key, shape, jnp.float32) * width * loudness
    return jnp.minimum(jnp.maximum(entries, -most), most).astype(dtype)


def setup_inputs(seed: int = 0) -> dict:
    streams_of = jax.random.split(jax.random.key(seed), 14)
    tokens = scatter_about(streams_of[0], (N_TP, SEQS // MIXER_HEADS, D // ROW_BLOCKS), 1.0, 6.0, ((0, 1024),))
    block_norm_gain = jnp.clip(1.0 + 0.18 * jax.random.normal(streams_of[1], (WINDOW_LAYERS, D), jnp.float32), 0.1, 1.9)
    receptance_weight = scatter_about(streams_of[2], (WINDOW_LAYERS, N_TP, D // ROW_BLOCKS, HEAD_CHANNELS), D ** -0.5, 0.09375, ((1, 1024),))
    key_weight = scatter_about(streams_of[3], (WINDOW_LAYERS, N_TP, D // ROW_BLOCKS, HEAD_CHANNELS), D ** -0.5, 0.09375, ((1, 1024),))
    value_weight = scatter_about(streams_of[4], (WINDOW_LAYERS, N_TP, D // ROW_BLOCKS, HEAD_CHANNELS), D ** -0.5, 0.09375, ((1, 1024),))
    decay_weight = scatter_about(streams_of[5], (WINDOW_LAYERS, N_TP, D // ROW_BLOCKS, HEAD_CHANNELS), D ** -0.5, 0.09375, ((1, 1024),))
    learning_rate_weight = scatter_about(streams_of[6], (WINDOW_LAYERS, N_TP, D // ROW_BLOCKS, HEAD_CHANNELS), D ** -0.5, 0.09375, ((1, 1024),))
    gate_weight = scatter_about(streams_of[7], (WINDOW_LAYERS, N_TP, D // ROW_BLOCKS, HEAD_CHANNELS), D ** -0.5, 0.09375, ((1, 1024),))
    decay_bias_fixed = jnp.clip(jax.random.uniform(streams_of[8], (WINDOW_LAYERS, MIXER_WIDTH), jnp.float32, -5.0, 2.0), -5.0, 2.0)
    self_token_weight = scatter_about(streams_of[9], (WINDOW_LAYERS, MIXER_WIDTH), 0.3, 1.5, (), jnp.float32)
    readout_norm_gain = jnp.clip(1.0 + 0.18 * jax.random.normal(streams_of[10], (WINDOW_LAYERS, MIXER_WIDTH), jnp.float32), 0.1, 1.9)
    output_weight = scatter_about(streams_of[11], (WINDOW_LAYERS, N_TP, HEAD_CHANNELS, D // ROW_BLOCKS), MIXER_WIDTH ** -0.5, 0.125, ((1, 1024),))
    state = scatter_about(streams_of[12], (WINDOW_LAYERS, N_TP, SEQS // ROW_BLOCKS, HEAD_CHANNELS * HEAD_CHANNELS), 0.5, 3.0, ((1, 1024),), jnp.float32)
    return {"tokens": tokens, "block_norm_gain": block_norm_gain, "receptance_weight": receptance_weight, "key_weight": key_weight, "value_weight": value_weight, "decay_weight": decay_weight, "learning_rate_weight": learning_rate_weight, "gate_weight": gate_weight, "decay_bias_fixed": decay_bias_fixed, "self_token_weight": self_token_weight, "readout_norm_gain": readout_norm_gain, "output_weight": output_weight, "state": state}


RMS_EPS = 1e-06
GROUP_EPS = 0.00064

def recurrent_update(layer_state, receptance_vector, key_vector, value_vector, decay_logits, learning_rate_logits, gate_logits, decay_constant, self_term_scale, head_gain_slice):
    highest = lax.Precision.HIGHEST
    shrink = jnp.exp(-jnp.exp(-jax.nn.softplus(-(decay_constant + decay_logits)) - 0.5))
    rate = jax.nn.sigmoid(learning_rate_logits)
    normed = key_vector * lax.rsqrt(lax.optimization_barrier(jnp.sum(key_vector * key_vector, -1, keepdims=True)) + 1.0)
    removed = jnp.einsum('...ij,...j->...i', layer_state, normed, precision=highest)
    layer_state = layer_state * shrink[..., None, :] - removed[..., :, None] * (normed * rate)[..., None, :] + value_vector[..., :, None] * (key_vector * rate)[..., None, :]
    readout = jnp.einsum('...ij,...j->...i', layer_state, receptance_vector, precision=highest)
    center = lax.optimization_barrier(jnp.mean(readout, -1, keepdims=True))
    spread = lax.optimization_barrier(jnp.mean(jnp.square(readout - center), -1, keepdims=True))
    normed_output = (readout - center) * lax.rsqrt(spread + GROUP_EPS) * head_gain_slice
    self_term = lax.optimization_barrier(jnp.sum(receptance_vector * key_vector * self_term_scale, -1, keepdims=True)) * value_vector
    return (((normed_output + self_term) * jax.nn.sigmoid(gate_logits)).astype(jnp.bfloat16), layer_state)

def reference(tokens, block_norm_gain, receptance_weight, key_weight, value_weight, decay_weight, learning_rate_weight, gate_weight, decay_bias_fixed, self_token_weight, readout_norm_gain, output_weight, state):
    seq_tile = SEQS // MIXER_HEADS
    col_tile = D // ROW_BLOCKS
    seq_block = SEQS // ROW_BLOCKS
    resid = tokens.reshape(MIXER_HEADS, ROW_BLOCKS, seq_tile, col_tile).transpose(0, 2, 1, 3).reshape(SEQS, D)

    def rows_full(weight):
        return weight.reshape(WINDOW_LAYERS, MIXER_HEADS, ROW_BLOCKS, col_tile, HEAD_CHANNELS).transpose(0, 2, 3, 1, 4).reshape(WINDOW_LAYERS, D, MIXER_WIDTH)
    fulls = [rows_full(weight) for weight in (receptance_weight, key_weight, value_weight, decay_weight, learning_rate_weight, gate_weight)]
    out_full = output_weight.reshape(WINDOW_LAYERS, MIXER_HEADS, ROW_BLOCKS, HEAD_CHANNELS, col_tile).transpose(0, 1, 3, 2, 4).reshape(WINDOW_LAYERS, MIXER_WIDTH, D)
    layer_states_stacked = state.reshape(WINDOW_LAYERS, MIXER_HEADS, ROW_BLOCKS, seq_block, HEAD_CHANNELS, HEAD_CHANNELS).transpose(0, 2, 3, 1, 4, 5)
    layer_states_stacked = layer_states_stacked.reshape(WINDOW_LAYERS, SEQS, MIXER_HEADS, HEAD_CHANNELS, HEAD_CHANNELS)
    updated = []
    for layer_index in range(WINDOW_LAYERS):
        wide = resid.astype(jnp.float32)
        scaled = (wide * block_norm_gain[layer_index]).astype(jnp.bfloat16)
        factor = lax.rsqrt(lax.optimization_barrier(jnp.mean(wide * wide, axis=1, keepdims=True)) + RMS_EPS)
        output_pieces = [(jnp.dot(scaled, full[layer_index], preferred_element_type=jnp.float32) * factor).reshape(SEQS, MIXER_HEADS, HEAD_CHANNELS) for full in fulls]
        head_results, layer_state = recurrent_update(layer_states_stacked[layer_index], *output_pieces, decay_bias_fixed[layer_index].reshape(MIXER_HEADS, HEAD_CHANNELS), self_token_weight[layer_index].reshape(MIXER_HEADS, HEAD_CHANNELS), readout_norm_gain[layer_index].reshape(MIXER_HEADS, HEAD_CHANNELS))
        branch = jnp.dot(head_results.reshape(SEQS, MIXER_WIDTH), out_full[layer_index], preferred_element_type=jnp.float32)
        resid = (wide + branch).astype(jnp.bfloat16)
        updated.append(layer_state)
    mixed = resid.reshape(MIXER_HEADS, seq_tile, ROW_BLOCKS, col_tile).transpose(0, 2, 1, 3).reshape(N_TP, seq_tile, col_tile)
    new_state = jnp.stack(updated).reshape(WINDOW_LAYERS, ROW_BLOCKS, seq_block, MIXER_HEADS, HEAD_CHANNELS, HEAD_CHANNELS).transpose(0, 3, 1, 2, 4, 5)
    new_state = new_state.reshape(WINDOW_LAYERS, N_TP, seq_block, HEAD_CHANNELS * HEAD_CHANNELS)
    return (mixed, new_state)
```

```python
import functools
import math

import jax
import jax.numpy as jnp
from jax import lax
from jax.experimental import pallas as pl
from jax.experimental.pallas import tpu as pltpu
from jax.sharding import PartitionSpec as P

D = 4096
RMS_EPS = 1e-06
GROUP_EPS = 0.00064
MESH = pl.DeviceIdType.MESH
F32 = jnp.float32
BF16 = jnp.bfloat16


def both_halves(tile, low):
    turned = pltpu.roll(tile, 64, 1)
    return jnp.where(low, tile, turned), jnp.where(low, turned, tile)


def half_sums(values, ones):
    flat = values.reshape(256, 128)
    high = flat.astype(BF16)
    rest = (flat - high.astype(F32)).astype(BF16)
    total = jnp.dot(high, ones, preferred_element_type=F32)
    total = total + jnp.dot(rest, ones, preferred_element_type=F32)
    return total.reshape(32, 8, 128)


def kernel(
    tokens,
    gain,
    w0,
    w1,
    w2,
    w3,
    w4,
    w5,
    bias,
    selfw,
    rgain,
    wout,
    state,
    mixed,
    new_state,
    xt,
    xbuf,
    wraw,
    wq,
    pbuf,
    rbuf,
    osend,
    obuf,
    wo,
    st,
    sn,
    vgain,
    vbias,
    vself,
    vrgain,
    lsem,
    ssem,
    rsem,
):
    me = lax.axis_index("tp")
    h = lax.div(me, 32)
    b = lax.rem(me, 32)
    core = lax.rem(me, 2)
    x = lax.rem(lax.div(me, 2), 8)
    ylo = lax.rem(lax.div(me, 16), 2)
    z2 = lax.div(h, 16)
    hx = lax.rem(lax.div(h, 2), 8)
    h0 = lax.rem(h, 2)
    jq = ylo * 2 + core

    loads = []

    def load(src, dst, sem):
        copy = pltpu.make_async_copy(src, dst, sem)
        copy.start()
        loads.append(copy)
        return copy

    tok_load = load(tokens.at[0], xt.at[0], lsem.at[0])
    w_loads = []
    for layer in range(2):
        for i, w in enumerate((w0, w1, w2, w3, w4, w5)):
            w_loads.append(load(w.at[layer, 0], wraw.at[layer, i], lsem.at[1 + layer * 6 + i]))
    wo_loads = [load(wout.at[l, 0], wo.at[l, h], lsem.at[13 + l]) for l in range(2)]
    gain_load = load(gain, vgain, lsem.at[15])
    bias_load = load(bias, vbias, lsem.at[16])
    self_load = load(selfw, vself, lsem.at[17])
    rgain_load = load(rgain, vrgain, lsem.at[18])
    st_loads = [load(state.at[l, 0], st.at[l], lsem.at[19 + l]) for l in range(2)]

    def tile_dest(i):
        other = lax.rem(h + 16 + i, 32)
        return other * 32 + z2 * 16 + x * 2 + h0

    def tile_source(i):
        return (ylo * 16 + lax.div(i, 4) * 2 + core) * 32 + lax.div(lax.rem(i, 4), 2) * 16 + x * 2 + lax.rem(i, 2)

    def x_partner(d):
        return me - x * 2 + lax.rem(x + d, 8) * 2

    def quad_partner(d):
        other = lax.rem(jq + d, 4)
        return me - ylo * 16 - core + lax.div(other, 2) * 16 + lax.rem(other, 2)

    def owner_dest(i):
        return b * 32 + lax.rem(lax.rem(me, 32) + 16 + i, 32)

    def head_partner(i):
        return lax.rem(h + i, 32) * 32 + b

    tile_self = jnp.logical_and(z2 == ylo, h0 == core)
    owner_self = h == b

    barrier = pltpu.get_barrier_semaphore()

    def greet(device):
        pl.semaphore_signal(barrier, inc=1, device_id=(device,), device_id_type=MESH)

    def greet_source(i, carry):
        @pl.when(tile_source(i) != me)
        def _():
            greet(tile_source(i))

        return carry

    lax.fori_loop(0, 32, greet_source, 0)
    for d in range(1, 8):
        greet(x_partner(d))
    for d in range(1, 4):
        greet(quad_partner(d))

    def own_weights(layer):
        for i in range(3):
            w_loads[layer * 6 + 2 * i].wait()
            w_loads[layer * 6 + 2 * i + 1].wait()
            pair = jnp.concatenate([wraw[layer, 2 * i], wraw[layer, 2 * i + 1]], axis=1)
            wq[layer, jq, :, 128 * i : 128 * i + 128] = pair

    own_weights(0)
    own_weights(1)
    tok_load.wait()

    @pl.when(tile_self)
    def _():
        pl.semaphore_wait(barrier, 41)

    @pl.when(jnp.logical_not(tile_self))
    def _():
        pl.semaphore_wait(barrier, 42)

    lane = lax.broadcasted_iota(jnp.int32, (8, 128), 1)
    low = lane < 64
    tile3 = lax.broadcasted_iota(jnp.int32, (32, 8, 128), 0)
    lane3 = lax.broadcasted_iota(jnp.int32, (32, 8, 128), 2)
    pick = jnp.logical_or(lane3 == 2 * tile3, lane3 == 2 * tile3 + 65)
    row_half = lax.broadcasted_iota(jnp.int32, (128, 128), 0) < 64
    col_half = lax.broadcasted_iota(jnp.int32, (128, 128), 1) < 64
    ones = jnp.where(row_half == col_half, 1.0, 0.0).astype(BF16)

    def remote(src, dst, phase, layer, device):
        return pltpu.make_async_remote_copy(
            src_ref=src,
            dst_ref=dst,
            send_sem=ssem.at[layer, phase],
            recv_sem=rsem.at[layer, phase],
            device_id=(device,),
            device_id_type=MESH,
        )

    def send_tiles(layer):
        slot = hx * 4 + jq

        def body(i, carry):
            dest = tile_dest(i)

            @pl.when(dest != me)
            def _():
                remote(xt.at[layer], xbuf.at[layer, slot], 0, layer, dest).start()

            return carry

        lax.fori_loop(0, 32, body, 0)

        @pl.when(tile_self)
        def _():
            xbuf[layer, slot] = xt[layer]

    def wait_bytes(ref, sem):
        pltpu.make_async_copy(ref, ref, sem).wait()

    def wait_counted(buf, layer, sem, fewer):
        @pl.when(fewer)
        def _():
            wait_bytes(buf.at[layer, pl.ds(0, 31)], sem)

        @pl.when(jnp.logical_not(fewer))
        def _():
            wait_bytes(buf.at[layer], sem)

    def send_quad(layer):
        for d in range(1, 4):
            remote(wq.at[layer, jq], wq.at[layer, jq], 3, layer, quad_partner(d)).start()

    def send_wout(layer):
        wo_loads[layer].wait()

        def body(i, carry):
            remote(wo.at[layer, h], wo.at[layer, h], 4, layer, head_partner(i)).start()
            return carry

        lax.fori_loop(1, 32, body, 0)

    def head_row(table, layer):
        row = table[layer : layer + 1, pl.ds(pl.multiple_of(lax.div(h, 2) * 128, 128), 128)]
        row = jnp.broadcast_to(row, (8, 128))
        first, second = both_halves(row, low)
        return jnp.where(h0 == 0, first, second)

    def project(layer):
        parts = []
        squares = jnp.zeros((64, 128), F32)
        for j in range(4):
            column = (j // 2) * 16 + x * 2 + j % 2
            wide = jnp.concatenate([xbuf[layer, s * 4 + j].astype(F32) for s in range(8)], axis=0)
            scale = vgain[layer : layer + 1, pl.ds(pl.multiple_of(column * 128, 128), 128)]
            parts.append((wide * scale).astype(BF16))
            squares = squares + wide * wide
        scaled = jnp.concatenate(parts, axis=1)
        wait_bytes(wq.at[layer, pl.ds(0, 3)], rsem.at[layer, 3])
        partial = jnp.dot(scaled, wq[layer].reshape(512, 384), preferred_element_type=F32)
        for s in range(8):
            pbuf[layer, s, :, 0:384] = partial[s * 8 : s * 8 + 8].astype(BF16)
            pbuf[layer, s, :, 384:512] = squares[s * 8 : s * 8 + 8].astype(BF16)
        for d in (4, 3, 5, 2, 6, 1, 7):
            to = lax.rem(x + d, 8)
            remote(pbuf.at[layer, to], rbuf.at[layer, x], 1, layer, x_partner(d)).start()
        rbuf[layer, x] = pbuf[layer, x]

    def recur(layer):
        wait_bytes(rbuf.at[layer, pl.ds(0, 7)], rsem.at[layer, 1])
        total = rbuf[layer, 0].astype(F32)
        for s in range(1, 8):
            total = total + rbuf[layer, s].astype(F32)
        mean_sq = jnp.sum(total[:, 384:512], axis=1, keepdims=True) / D
        projected = total[:, 0:384] * lax.rsqrt(mean_sq + RMS_EPS)
        r, k = both_halves(projected[:, 0:128], low)
        v, p = both_halves(projected[:, 128:256], low)
        q, g = both_halves(projected[:, 256:384], low)
        decay = jnp.exp(-math.exp(-0.5) * jax.nn.sigmoid(head_row(vbias, layer) + p))
        rate = jax.nn.sigmoid(q)
        kn = k * lax.rsqrt(jnp.sum(k * k, axis=1, keepdims=True) * 0.5 + 1.0)
        st_loads[layer].wait()
        old = jnp.stack([st[layer, :, 128 * t : 128 * t + 128] for t in range(32)])
        removed = half_sums(old * kn[None], ones)
        vs = half_sums(jnp.where(pick, v[None], 0.0), ones)
        new = old * decay[None] - removed * (kn * rate)[None] + vs * (k * rate)[None]
        for t in range(32):
            sn[layer, :, 128 * t : 128 * t + 128] = new[t]
        reads = half_sums(new * r[None], ones)
        read = jnp.sum(jnp.where(pick, reads, 0.0), axis=0)
        read = read + pltpu.roll(read, 64, 1)
        center = read - jnp.sum(read, axis=1, keepdims=True) / 128
        spread = jnp.sum(center * center, axis=1, keepdims=True) / 128
        normed = center * lax.rsqrt(spread + GROUP_EPS) * head_row(vrgain, layer)
        own = jnp.sum(r * k * head_row(vself, layer), axis=1, keepdims=True) * 0.5
        out = (normed + own * v) * jax.nn.sigmoid(g)
        osend[layer] = out.astype(BF16)

        def body(i, carry):
            dest = owner_dest(i)

            @pl.when(dest != me)
            def _():
                remote(osend.at[layer], obuf.at[layer, h], 2, layer, dest).start()

            return carry

        lax.fori_loop(0, 32, body, 0)

        @pl.when(owner_self)
        def _():
            obuf[layer, h] = osend[layer]

        pltpu.make_async_copy(sn.at[layer], new_state.at[layer, 0], lsem.at[21 + layer]).start()

    def combine(layer):
        wait_bytes(wo.at[layer, pl.ds(0, 31)], rsem.at[layer, 4])
        wait_counted(obuf, layer, rsem.at[layer, 2], owner_self)
        pieces = []
        for i in range(16):
            even = obuf[layer, 2 * i].astype(F32)
            odd = obuf[layer, 2 * i + 1].astype(F32)
            pieces.append(jnp.where(low, even, odd).astype(BF16))
        heads = jnp.concatenate(pieces, axis=1)
        branch = jnp.dot(heads, wo[layer].reshape(2048, 128), preferred_element_type=F32)
        return (xt[layer].astype(F32) + branch).astype(BF16)

    send_tiles(0)
    send_quad(0)
    send_quad(1)
    gain_load.wait()
    bias_load.wait()
    self_load.wait()
    rgain_load.wait()
    for layer in range(2):
        wait_counted(xbuf, layer, rsem.at[layer, 0], tile_self)
        send_wout(layer)
        project(layer)
        recur(layer)
        tile = combine(layer)
        if layer == 0:
            xt[1] = tile
            send_tiles(1)
        else:
            mixed[0] = tile

    for layer in range(2):
        wait_counted(xbuf, layer, ssem.at[layer, 0], tile_self)
        wait_bytes(rbuf.at[layer, pl.ds(0, 7)], ssem.at[layer, 1])
        wait_counted(obuf, layer, ssem.at[layer, 2], owner_self)
        wait_bytes(wq.at[layer, pl.ds(0, 3)], ssem.at[layer, 3])
        wait_bytes(wo.at[layer, pl.ds(0, 31)], ssem.at[layer, 4])
        pltpu.make_async_copy(sn.at[layer], new_state.at[layer, 0], lsem.at[21 + layer]).wait()


def on_device(*args):
    anywhere = pl.BlockSpec(memory_space=pl.ANY)
    return pl.pallas_call(
        kernel,
        out_shape=(
            jax.ShapeDtypeStruct((1, 8, 128), BF16),
            jax.ShapeDtypeStruct((2, 1, 8, 4096), F32),
        ),
        in_specs=[anywhere] * 13,
        out_specs=(pl.BlockSpec(memory_space=pltpu.VMEM), anywhere),
        scratch_shapes=[
            pltpu.VMEM((2, 8, 128), BF16),
            pltpu.VMEM((2, 32, 8, 128), BF16),
            pltpu.VMEM((2, 6, 128, 64), BF16),
            pltpu.VMEM((2, 4, 128, 384), BF16),
            pltpu.VMEM((2, 8, 8, 512), BF16),
            pltpu.VMEM((2, 8, 8, 512), BF16),
            pltpu.VMEM((2, 8, 128), BF16),
            pltpu.VMEM((2, 32, 8, 128), BF16),
            pltpu.VMEM((2, 32, 64, 128), BF16),
            pltpu.VMEM((2, 8, 4096), F32),
            pltpu.VMEM((2, 8, 4096), F32),
            pltpu.VMEM((2, 4096), F32),
            pltpu.VMEM((2, 2048), F32),
            pltpu.VMEM((2, 2048), F32),
            pltpu.VMEM((2, 2048), F32),
            pltpu.SemaphoreType.DMA((23,)),
            pltpu.SemaphoreType.DMA((2, 5)),
            pltpu.SemaphoreType.DMA((2, 5)),
        ],
        compiler_params=pltpu.CompilerParams(collective_id=0, has_side_effects=True),
    )(*args)


def solution(mesh):
    weight = P(None, "tp", None, None)
    return jax.shard_map(
        on_device,
        mesh=mesh,
        in_specs=(
            P("tp", None, None),
            P(),
            weight,
            weight,
            weight,
            weight,
            weight,
            weight,
            P(),
            P(),
            P(),
            weight,
            weight,
        ),
        out_specs=(P("tp", None, None), weight),
        check_vma=False,
    )
```

```python
import functools
import math

import jax
import jax.numpy as jnp
from jax import lax
from jax.experimental import pallas as pl
from jax.experimental.pallas import tpu as pltpu
from jax.sharding import PartitionSpec as P

D = 4096
RMS_EPS = 1e-06
GROUP_EPS = 0.00064
MESH = pl.DeviceIdType.MESH
F32 = jnp.float32
BF16 = jnp.bfloat16


def both_halves(tile, low):
    turned = pltpu.roll(tile, 64, 1)
    return jnp.where(low, tile, turned), jnp.where(low, turned, tile)


def half_sums(values, ones):
    flat = values.reshape(256, 128)
    high = flat.astype(BF16)
    rest = (flat - high.astype(F32)).astype(BF16)
    total = jnp.dot(high, ones, preferred_element_type=F32)
    total = total + jnp.dot(rest, ones, preferred_element_type=F32)
    return total.reshape(32, 8, 128)


def kernel(
    tokens,
    gain,
    w0,
    w1,
    w2,
    w3,
    w4,
    w5,
    bias,
    selfw,
    rgain,
    wout,
    state,
    mixed,
    new_state,
    xt,
    xbuf,
    wq,
    pbuf,
    rbuf,
    osend,
    obuf,
    wo,
    st,
    sn,
    vgain,
    vbias,
    vself,
    vrgain,
    lsem,
    ssem,
    rsem,
):
    me = lax.axis_index("tp")
    h = lax.div(me, 32)
    b = lax.rem(me, 32)
    core = lax.rem(me, 2)
    x = lax.rem(lax.div(me, 2), 8)
    ylo = lax.rem(lax.div(me, 16), 2)
    z = lax.div(h, 4)
    z2 = lax.div(h, 16)
    hx = lax.rem(lax.div(h, 2), 8)
    h0 = lax.rem(h, 2)
    jq = ylo * 2 + core

    loads = []

    def load(src, dst, sem):
        copy = pltpu.make_async_copy(src, dst, sem)
        copy.start()
        loads.append(copy)
        return copy

    tok_load = load(tokens.at[0], xt.at[0], lsem.at[0])
    w_loads = []
    for layer in range(2):
        for i, w in enumerate((w0, w1, w2, w3, w4, w5)):
            w_loads.append(load(w.at[layer, 0], wq.at[layer, jq, pl.ds(64 * i, 64)], lsem.at[1 + layer * 6 + i]))
    wo_loads = [load(wout.at[l, 0], wo.at[l, h], lsem.at[13 + l]) for l in range(2)]
    gain_load = load(gain, vgain, lsem.at[15])
    bias_load = load(bias, vbias, lsem.at[16])
    self_load = load(selfw, vself, lsem.at[17])
    rgain_load = load(rgain, vrgain, lsem.at[18])
    st_loads = [load(state.at[l, 0], st.at[l], lsem.at[19 + l]) for l in range(2)]

    def tile_dest(i):
        other = lax.rem(h + 16 + i, 32)
        return other * 32 + z2 * 16 + x * 2 + h0

    def tile_source(i):
        return (ylo * 16 + lax.div(i, 4) * 2 + core) * 32 + lax.div(lax.rem(i, 4), 2) * 16 + x * 2 + lax.rem(i, 2)

    def x_partner(d):
        return me - x * 2 + lax.rem(x + d, 8) * 2

    def quad_partner(d):
        other = lax.rem(jq + d, 4)
        return me - ylo * 16 - core + lax.div(other, 2) * 16 + lax.rem(other, 2)

    def owner_dest(i):
        return b * 32 + lax.rem(lax.rem(me, 32) + 16 + i, 32)

    def y_partner(d):
        return (z * 4 + lax.rem(h + d, 4)) * 32 + b

    def z_partner(d):
        return lax.rem(me + d * 128, 1024)

    tile_self = jnp.logical_and(z2 == ylo, h0 == core)
    owner_self = h == b

    barrier = pltpu.get_barrier_semaphore()

    def greet(device):
        pl.semaphore_signal(barrier, inc=1, device_id=(device,), device_id_type=MESH)

    def greet_source(i, carry):
        @pl.when(tile_source(i) != me)
        def _():
            greet(tile_source(i))

        return carry

    lax.fori_loop(0, 32, greet_source, 0)
    for d in range(1, 8):
        greet(x_partner(d))
    for d in range(1, 4):
        greet(quad_partner(d))
        greet(y_partner(d))

    tok_load.wait()

    @pl.when(tile_self)
    def _():
        pl.semaphore_wait(barrier, 44)

    @pl.when(jnp.logical_not(tile_self))
    def _():
        pl.semaphore_wait(barrier, 45)

    lane = lax.broadcasted_iota(jnp.int32, (8, 128), 1)
    low = lane < 64
    tile3 = lax.broadcasted_iota(jnp.int32, (32, 8, 128), 0)
    lane3 = lax.broadcasted_iota(jnp.int32, (32, 8, 128), 2)
    pick = jnp.logical_or(lane3 == 2 * tile3, lane3 == 2 * tile3 + 65)
    row_half = lax.broadcasted_iota(jnp.int32, (128, 128), 0) < 64
    col_half = lax.broadcasted_iota(jnp.int32, (128, 128), 1) < 64
    ones = jnp.where(row_half == col_half, 1.0, 0.0).astype(BF16)

    def remote(src, dst, phase, layer, device):
        return pltpu.make_async_remote_copy(
            src_ref=src,
            dst_ref=dst,
            send_sem=ssem.at[layer, phase],
            recv_sem=rsem.at[layer, phase],
            device_id=(device,),
            device_id_type=MESH,
        )

    def send_all(start):
        def first(i, carry):
            for k in range(4):
                start(i * 4 + k)
            return carry

        def second(i, carry):
            for k in range(3):
                start(17 + i * 3 + k)
            return carry

        lax.fori_loop(0, 4, first, 0)
        lax.fori_loop(0, 5, second, 0)

    def send_tiles(layer):
        slot = hx * 4 + jq

        def start(i):
            remote(xt.at[layer], xbuf.at[layer, slot], 0, layer, tile_dest(i)).start()

        send_all(start)

        @pl.when(tile_self)
        def _():
            xbuf[layer, slot] = xt[layer]

        @pl.when(jnp.logical_not(tile_self))
        def _():
            start(16)

    def wait_bytes(ref, sem):
        pltpu.make_async_copy(ref, ref, sem).wait()

    def wait_counted(buf, layer, sem, fewer):
        @pl.when(fewer)
        def _():
            wait_bytes(buf.at[layer, pl.ds(0, 31)], sem)

        @pl.when(jnp.logical_not(fewer))
        def _():
            wait_bytes(buf.at[layer], sem)

    def send_quad(layer):
        for i in range(6):
            w_loads[layer * 6 + i].wait()
        for d in range(1, 4):
            remote(wq.at[layer, jq], wq.at[layer, jq], 3, layer, quad_partner(d)).start()

    def send_wout_y(layer):
        wo_loads[layer].wait()
        for d in (2, 1, 3):
            remote(wo.at[layer, h], wo.at[layer, h], 4, layer, y_partner(d)).start()

    def send_wout_z(layer):
        wait_bytes(wo.at[layer, pl.ds(0, 3)], rsem.at[layer, 4])
        block = wo.at[layer, pl.ds(z * 4, 4)]
        for d in (4, 3, 5, 2, 6, 1, 7):
            remote(block, block, 5, layer, z_partner(d)).start()

    def head_row(table, layer):
        row = table[layer : layer + 1, pl.ds(pl.multiple_of(lax.div(h, 2) * 128, 128), 128)]
        row = jnp.broadcast_to(row, (8, 128))
        first, second = both_halves(row, low)
        return jnp.where(h0 == 0, first, second)

    def project(layer):
        wait_bytes(wq.at[layer, pl.ds(0, 3)], rsem.at[layer, 3])
        partial = jnp.zeros((64, 384), F32)
        squares = jnp.zeros((64, 128), F32)
        for j in range(4):
            column = (j // 2) * 16 + x * 2 + j % 2
            wide = jnp.concatenate([xbuf[layer, s * 4 + j].astype(F32) for s in range(8)], axis=0)
            scale = vgain[layer : layer + 1, pl.ds(pl.multiple_of(column * 128, 128), 128)]
            partial = partial + lax.dot_general(
                (wide * scale).astype(BF16),
                wq[layer, j],
                (((1,), (1,)), ((), ())),
                preferred_element_type=F32,
            )
            squares = squares + wide * wide
        for s in range(8):
            pbuf[layer, s, :, 0:384] = partial[s * 8 : s * 8 + 8].astype(BF16)
            pbuf[layer, s, :, 384:512] = squares[s * 8 : s * 8 + 8].astype(BF16)
        for d in (4, 3, 5, 2, 6, 1, 7):
            to = lax.rem(x + d, 8)
            remote(pbuf.at[layer, to], rbuf.at[layer, x], 1, layer, x_partner(d)).start()
        rbuf[layer, x] = pbuf[layer, x]

    def recur(layer):
        wait_bytes(rbuf.at[layer, pl.ds(0, 7)], rsem.at[layer, 1])
        total = rbuf[layer, 0].astype(F32)
        for s in range(1, 8):
            total = total + rbuf[layer, s].astype(F32)
        mean_sq = jnp.sum(total[:, 384:512], axis=1, keepdims=True) / D
        projected = total[:, 0:384] * lax.rsqrt(mean_sq + RMS_EPS)
        r, k = both_halves(projected[:, 0:128], low)
        v, p = both_halves(projected[:, 128:256], low)
        q, g = both_halves(projected[:, 256:384], low)
        decay = jnp.exp(-math.exp(-0.5) * jax.nn.sigmoid(head_row(vbias, layer) + p))
        rate = jax.nn.sigmoid(q)
        kn = k * lax.rsqrt(jnp.sum(k * k, axis=1, keepdims=True) * 0.5 + 1.0)
        st_loads[layer].wait()
        old = jnp.stack([st[layer, :, 128 * t : 128 * t + 128] for t in range(32)])
        removed = half_sums(old * kn[None], ones)
        vs = half_sums(jnp.where(pick, v[None], 0.0), ones)
        new = old * decay[None] - removed * (kn * rate)[None] + vs * (k * rate)[None]
        for t in range(32):
            sn[layer, :, 128 * t : 128 * t + 128] = new[t]
        reads = half_sums(new * r[None], ones)
        read = jnp.sum(jnp.where(pick, reads, 0.0), axis=0)
        read = read + pltpu.roll(read, 64, 1)
        center = read - jnp.sum(read, axis=1, keepdims=True) / 128
        spread = jnp.sum(center * center, axis=1, keepdims=True) / 128
        normed = center * lax.rsqrt(spread + GROUP_EPS) * head_row(vrgain, layer)
        own = jnp.sum(r * k * head_row(vself, layer), axis=1, keepdims=True) * 0.5
        out = (normed + own * v) * jax.nn.sigmoid(g)
        osend[layer] = out.astype(BF16)

        def start(i):
            remote(osend.at[layer], obuf.at[layer, h], 2, layer, owner_dest(i)).start()

        send_all(start)

        @pl.when(owner_self)
        def _():
            obuf[layer, h] = osend[layer]

        @pl.when(jnp.logical_not(owner_self))
        def _():
            start(16)

        pltpu.make_async_copy(sn.at[layer], new_state.at[layer, 0], lsem.at[21 + layer]).start()

    def combine(layer):
        wait_bytes(wo.at[layer, pl.ds(0, 28)], rsem.at[layer, 5])
        wait_counted(obuf, layer, rsem.at[layer, 2], owner_self)
        pieces = []
        for i in range(16):
            even = obuf[layer, 2 * i].astype(F32)
            odd = obuf[layer, 2 * i + 1].astype(F32)
            pieces.append(jnp.where(low, even, odd).astype(BF16))
        heads = jnp.concatenate(pieces, axis=1)
        branch = jnp.dot(heads, wo[layer].reshape(2048, 128), preferred_element_type=F32)
        return xt[layer].astype(F32) + branch

    send_tiles(0)
    send_quad(0)
    send_wout_y(0)
    send_wout_y(1)
    gain_load.wait()
    bias_load.wait()
    self_load.wait()
    rgain_load.wait()
    for layer in range(2):
        wait_counted(xbuf, layer, rsem.at[layer, 0], tile_self)
        if layer == 1:
            send_wout_z(1)
        project(layer)
        if layer == 0:
            send_wout_z(0)
            send_quad(1)
        recur(layer)
        tile = combine(layer)
        if layer == 0:
            xt[1] = tile.astype(BF16)
            send_tiles(1)
        else:
            mixed[0] = tile

    for layer in range(2):
        wait_counted(xbuf, layer, ssem.at[layer, 0], tile_self)
        wait_bytes(rbuf.at[layer, pl.ds(0, 7)], ssem.at[layer, 1])
        wait_counted(obuf, layer, ssem.at[layer, 2], owner_self)
        wait_bytes(wq.at[layer, pl.ds(0, 3)], ssem.at[layer, 3])
        wait_bytes(wo.at[layer, pl.ds(0, 3)], ssem.at[layer, 4])
        wait_bytes(wo.at[layer, pl.ds(0, 28)], ssem.at[layer, 5])
        pltpu.make_async_copy(sn.at[layer], new_state.at[layer, 0], lsem.at[21 + layer]).wait()


def on_device(*args):
    args = args[:2] + tuple(jnp.swapaxes(w, 2, 3) for w in args[2:8]) + args[8:]
    anywhere = pl.BlockSpec(memory_space=pl.ANY)
    mixed, new_state = pl.pallas_call(
        kernel,
        out_shape=(
            jax.ShapeDtypeStruct((1, 8, 128), F32),
            jax.ShapeDtypeStruct((2, 1, 8, 4096), F32),
        ),
        in_specs=[anywhere] * 13,
        out_specs=(pl.BlockSpec(memory_space=pltpu.VMEM), anywhere),
        scratch_shapes=[
            pltpu.VMEM((2, 8, 128), BF16),
            pltpu.VMEM((2, 32, 8, 128), BF16),
            pltpu.VMEM((2, 4, 384, 128), BF16),
            pltpu.VMEM((2, 8, 8, 512), BF16),
            pltpu.VMEM((2, 8, 8, 512), BF16),
            pltpu.VMEM((2, 8, 128), BF16),
            pltpu.VMEM((2, 32, 8, 128), BF16),
            pltpu.VMEM((2, 32, 64, 128), BF16),
            pltpu.VMEM((2, 8, 4096), F32),
            pltpu.VMEM((2, 8, 4096), F32),
            pltpu.VMEM((2, 4096), F32),
            pltpu.VMEM((2, 2048), F32),
            pltpu.VMEM((2, 2048), F32),
            pltpu.VMEM((2, 2048), F32),
            pltpu.SemaphoreType.DMA((23,)),
            pltpu.SemaphoreType.DMA((2, 6)),
            pltpu.SemaphoreType.DMA((2, 6)),
        ],
        compiler_params=pltpu.CompilerParams(collective_id=0, has_side_effects=True),
    )(*args)
    return mixed.astype(BF16), new_state


def solution(mesh):
    weight = P(None, "tp", None, None)
    return jax.shard_map(
        on_device,
        mesh=mesh,
        in_specs=(
            P("tp", None, None),
            P(),
            weight,
            weight,
            weight,
            weight,
            weight,
            weight,
            P(),
            P(),
            P(),
            weight,
            weight,
        ),
        out_specs=(P("tp", None, None), weight),
        check_vma=False,
    )
```

```python
import functools
import math

import jax
import jax.numpy as jnp
from jax import lax
from jax.experimental import pallas as pl
from jax.experimental.pallas import tpu as pltpu
from jax.sharding import PartitionSpec as P

D = 4096
RMS_EPS = 1e-06
GROUP_EPS = 0.00064
MESH = pl.DeviceIdType.MESH
F32 = jnp.float32
BF16 = jnp.bfloat16


def both_halves(tile, low):
    turned = pltpu.roll(tile, 64, 1)
    return jnp.where(low, tile, turned), jnp.where(low, turned, tile)


def half_sums(values, ones):
    flat = values.reshape(256, 128)
    high = flat.astype(BF16)
    rest = (flat - high.astype(F32)).astype(BF16)
    total = jnp.dot(high, ones, preferred_element_type=F32)
    total = total + jnp.dot(rest, ones, preferred_element_type=F32)
    return total.reshape(32, 8, 128)


def kernel(
    tokens,
    gain,
    w0,
    w1,
    w2,
    w3,
    w4,
    w5,
    bias,
    selfw,
    rgain,
    wout,
    state,
    mixed,
    new_state,
    xt,
    xbuf,
    wq,
    pbuf,
    rbuf,
    osend,
    obuf,
    wo,
    st,
    sn,
    vgain,
    vbias,
    vself,
    vrgain,
    lsem,
    ssem,
    rsem,
):
    me = lax.axis_index("tp")
    h = lax.div(me, 32)
    b = lax.rem(me, 32)
    core = lax.rem(me, 2)
    x = lax.rem(lax.div(me, 2), 8)
    ylo = lax.rem(lax.div(me, 16), 2)
    z = lax.div(h, 4)
    z2 = lax.div(h, 16)
    hx = lax.rem(lax.div(h, 2), 8)
    h0 = lax.rem(h, 2)
    jq = ylo * 2 + core

    loads = []

    def load(src, dst, sem):
        copy = pltpu.make_async_copy(src, dst, sem)
        copy.start()
        loads.append(copy)
        return copy

    tok_load = load(tokens.at[0], xt.at[0], lsem.at[0])

    def tile_dest(i):
        other = lax.rem(h + 16 + i, 32)
        return other * 32 + z2 * 16 + x * 2 + h0

    def tile_source(i):
        tile_head = ylo * 16 + lax.rem(lax.div(i, 4) + hx, 8) * 2 + core
        quad = lax.rem(i + jq, 4)
        return tile_head * 32 + lax.div(quad, 2) * 16 + x * 2 + lax.rem(quad, 2)

    def x_partner(d):
        return me - x * 2 + lax.rem(x + d, 8) * 2

    def quad_partner(d):
        other = lax.rem(jq + d, 4)
        return me - ylo * 16 - core + lax.div(other, 2) * 16 + lax.rem(other, 2)

    def owner_dest(i):
        return b * 32 + lax.rem(lax.rem(me, 32) + 16 + i, 32)

    def y_partner(d):
        return (z * 4 + lax.rem(h + d, 4)) * 32 + b

    def z_partner(d):
        return lax.rem(me + d * 128, 1024)

    tile_self = jnp.logical_and(z2 == ylo, h0 == core)
    owner_self = h == b

    barrier = pltpu.get_barrier_semaphore()

    def greet(device):
        pl.semaphore_signal(barrier, inc=1, device_id=(device,), device_id_type=MESH)

    def greet_sources(i, carry):
        for k in range(4):
            greet(tile_source(i * 4 + k))
        return carry

    lax.fori_loop(1, 8, greet_sources, 0)
    for i in range(1, 4):
        greet(tile_source(i))

    @pl.when(jnp.logical_not(tile_self))
    def _():
        greet(tile_source(0))

    for d in range(1, 8):
        greet(x_partner(d))
    for d in range(1, 4):
        greet(quad_partner(d))
        greet(y_partner(d))

    w_loads = []
    for layer in range(2):
        for i, w in enumerate((w0, w1, w2, w3, w4, w5)):
            w_loads.append(load(w.at[layer, 0], wq.at[layer, jq, pl.ds(64 * i, 64)], lsem.at[1 + layer * 6 + i]))
    wo_loads = [load(wout.at[l, 0], wo.at[l, h], lsem.at[13 + l]) for l in range(2)]
    gain_load = load(gain, vgain, lsem.at[15])
    bias_load = load(bias, vbias, lsem.at[16])
    self_load = load(selfw, vself, lsem.at[17])
    rgain_load = load(rgain, vrgain, lsem.at[18])
    st_loads = [load(state.at[l, 0], st.at[l], lsem.at[19 + l]) for l in range(2)]

    tok_load.wait()

    @pl.when(tile_self)
    def _():
        pl.semaphore_wait(barrier, 44)

    @pl.when(jnp.logical_not(tile_self))
    def _():
        pl.semaphore_wait(barrier, 45)

    lane = lax.broadcasted_iota(jnp.int32, (8, 128), 1)
    low = lane < 64
    tile3 = lax.broadcasted_iota(jnp.int32, (32, 8, 128), 0)
    lane3 = lax.broadcasted_iota(jnp.int32, (32, 8, 128), 2)
    pick = jnp.logical_or(lane3 == 2 * tile3, lane3 == 2 * tile3 + 65)
    row_half = lax.broadcasted_iota(jnp.int32, (128, 128), 0) < 64
    col_half = lax.broadcasted_iota(jnp.int32, (128, 128), 1) < 64
    ones = jnp.where(row_half == col_half, 1.0, 0.0).astype(BF16)

    def remote(src, dst, phase, layer, device):
        return pltpu.make_async_remote_copy(
            src_ref=src,
            dst_ref=dst,
            send_sem=ssem.at[layer, phase],
            recv_sem=rsem.at[layer, phase],
            device_id=(device,),
            device_id_type=MESH,
        )

    def send_all(start):
        def first(i, carry):
            for k in range(4):
                start(i * 4 + k)
            return carry

        def second(i, carry):
            for k in range(3):
                start(17 + i * 3 + k)
            return carry

        lax.fori_loop(0, 4, first, 0)
        lax.fori_loop(0, 5, second, 0)

    def send_tiles(layer):
        slot = hx * 4 + jq

        def start(i):
            remote(xt.at[layer], xbuf.at[layer, slot], 0, layer, tile_dest(i)).start()

        send_all(start)

        @pl.when(tile_self)
        def _():
            xbuf[layer, slot] = xt[layer]

        @pl.when(jnp.logical_not(tile_self))
        def _():
            start(16)

    def wait_bytes(ref, sem):
        pltpu.make_async_copy(ref, ref, sem).wait()

    def wait_counted(buf, layer, sem, fewer):
        @pl.when(fewer)
        def _():
            wait_bytes(buf.at[layer, pl.ds(0, 31)], sem)

        @pl.when(jnp.logical_not(fewer))
        def _():
            wait_bytes(buf.at[layer], sem)

    def send_quad(layer):
        for i in range(6):
            w_loads[layer * 6 + i].wait()
        for d in range(1, 4):
            remote(wq.at[layer, jq], wq.at[layer, jq], 3, layer, quad_partner(d)).start()

    def send_wout_y(layer):
        wo_loads[layer].wait()
        for d in (2, 1, 3):
            remote(wo.at[layer, h], wo.at[layer, h], 4, layer, y_partner(d)).start()

    def send_wout_z(layer):
        wait_bytes(wo.at[layer, pl.ds(0, 3)], rsem.at[layer, 4])
        block = wo.at[layer, pl.ds(z * 4, 4)]
        for d in (4, 3, 5, 2, 6, 1, 7):
            remote(block, block, 5, layer, z_partner(d)).start()

    def head_row(table, layer):
        row = table[layer : layer + 1, pl.ds(pl.multiple_of(lax.div(h, 2) * 128, 128), 128)]
        row = jnp.broadcast_to(row, (8, 128))
        first, second = both_halves(row, low)
        return jnp.where(h0 == 0, first, second)

    def project(layer):
        wait_bytes(wq.at[layer, pl.ds(0, 3)], rsem.at[layer, 3])
        partial = jnp.zeros((64, 384), F32)
        squares = jnp.zeros((64, 128), F32)
        for j in range(4):
            column = (j // 2) * 16 + x * 2 + j % 2
            wide = jnp.concatenate([xbuf[layer, s * 4 + j].astype(F32) for s in range(8)], axis=0)
            scale = vgain[layer : layer + 1, pl.ds(pl.multiple_of(column * 128, 128), 128)]
            partial = partial + lax.dot_general(
                (wide * scale).astype(BF16),
                wq[layer, j],
                (((1,), (1,)), ((), ())),
                preferred_element_type=F32,
            )
            squares = squares + wide * wide
        for s in range(8):
            pbuf[layer, s, :, 0:384] = partial[s * 8 : s * 8 + 8].astype(BF16)
            pbuf[layer, s, :, 384:512] = squares[s * 8 : s * 8 + 8].astype(BF16)
        for d in (4, 3, 5, 2, 6, 1, 7):
            to = lax.rem(x + d, 8)
            remote(pbuf.at[layer, to], rbuf.at[layer, x], 1, layer, x_partner(d)).start()
        rbuf[layer, x] = pbuf[layer, x]

    def recur(layer):
        wait_bytes(rbuf.at[layer, pl.ds(0, 7)], rsem.at[layer, 1])
        total = rbuf[layer, 0].astype(F32)
        for s in range(1, 8):
            total = total + rbuf[layer, s].astype(F32)
        mean_sq = jnp.sum(total[:, 384:512], axis=1, keepdims=True) / D
        projected = total[:, 0:384] * lax.rsqrt(mean_sq + RMS_EPS)
        r, k = both_halves(projected[:, 0:128], low)
        v, p = both_halves(projected[:, 128:256], low)
        q, g = both_halves(projected[:, 256:384], low)
        decay = jnp.exp(-math.exp(-0.5) * jax.nn.sigmoid(head_row(vbias, layer) + p))
        rate = jax.nn.sigmoid(q)
        kn = k * lax.rsqrt(jnp.sum(k * k, axis=1, keepdims=True) * 0.5 + 1.0)
        st_loads[layer].wait()
        old = jnp.stack([st[layer, :, 128 * t : 128 * t + 128] for t in range(32)])
        removed = half_sums(old * kn[None], ones)
        vs = half_sums(jnp.where(pick, v[None], 0.0), ones)
        new = old * decay[None] - removed * (kn * rate)[None] + vs * (k * rate)[None]
        for t in range(32):
            sn[layer, :, 128 * t : 128 * t + 128] = new[t]
        reads = half_sums(new * r[None], ones)
        read = jnp.sum(jnp.where(pick, reads, 0.0), axis=0)
        read = read + pltpu.roll(read, 64, 1)
        center = read - jnp.sum(read, axis=1, keepdims=True) / 128
        spread = jnp.sum(center * center, axis=1, keepdims=True) / 128
        normed = center * lax.rsqrt(spread + GROUP_EPS) * head_row(vrgain, layer)
        own = jnp.sum(r * k * head_row(vself, layer), axis=1, keepdims=True) * 0.5
        out = (normed + own * v) * jax.nn.sigmoid(g)
        osend[layer] = out.astype(BF16)

        def start(i):
            remote(osend.at[layer], obuf.at[layer, h], 2, layer, owner_dest(i)).start()

        send_all(start)

        @pl.when(owner_self)
        def _():
            obuf[layer, h] = osend[layer]

        @pl.when(jnp.logical_not(owner_self))
        def _():
            start(16)

        pltpu.make_async_copy(sn.at[layer], new_state.at[layer, 0], lsem.at[21 + layer]).start()

    def combine(layer):
        wait_bytes(wo.at[layer, pl.ds(0, 28)], rsem.at[layer, 5])
        wait_counted(obuf, layer, rsem.at[layer, 2], owner_self)
        pieces = []
        for i in range(16):
            even = obuf[layer, 2 * i].astype(F32)
            odd = obuf[layer, 2 * i + 1].astype(F32)
            pieces.append(jnp.where(low, even, odd).astype(BF16))
        heads = jnp.concatenate(pieces, axis=1)
        branch = jnp.dot(heads, wo[layer].reshape(2048, 128), preferred_element_type=F32)
        return xt[layer].astype(F32) + branch

    send_tiles(0)
    send_quad(0)
    send_wout_y(0)
    gain_load.wait()
    bias_load.wait()
    self_load.wait()
    rgain_load.wait()
    for layer in range(2):
        wait_counted(xbuf, layer, rsem.at[layer, 0], tile_self)
        if layer == 1:
            send_wout_z(1)
        project(layer)
        if layer == 0:
            send_wout_z(0)
            send_quad(1)
            send_wout_y(1)
        recur(layer)
        tile = combine(layer)
        if layer == 0:
            xt[1] = tile.astype(BF16)
            send_tiles(1)
        else:
            mixed[0] = tile

    for layer in range(2):
        wait_counted(xbuf, layer, ssem.at[layer, 0], tile_self)
        wait_bytes(rbuf.at[layer, pl.ds(0, 7)], ssem.at[layer, 1])
        wait_counted(obuf, layer, ssem.at[layer, 2], owner_self)
        wait_bytes(wq.at[layer, pl.ds(0, 3)], ssem.at[layer, 3])
        wait_bytes(wo.at[layer, pl.ds(0, 3)], ssem.at[layer, 4])
        wait_bytes(wo.at[layer, pl.ds(0, 28)], ssem.at[layer, 5])
        pltpu.make_async_copy(sn.at[layer], new_state.at[layer, 0], lsem.at[21 + layer]).wait()


def on_device(*args):
    args = args[:2] + tuple(jnp.swapaxes(w, 2, 3) for w in args[2:8]) + args[8:]
    anywhere = pl.BlockSpec(memory_space=pl.ANY)
    mixed, new_state = pl.pallas_call(
        kernel,
        out_shape=(
            jax.ShapeDtypeStruct((1, 8, 128), F32),
            jax.ShapeDtypeStruct((2, 1, 8, 4096), F32),
        ),
        in_specs=[anywhere] * 13,
        out_specs=(pl.BlockSpec(memory_space=pltpu.VMEM), anywhere),
        scratch_shapes=[
            pltpu.VMEM((2, 8, 128), BF16),
            pltpu.VMEM((2, 32, 8, 128), BF16),
            pltpu.VMEM((2, 4, 384, 128), BF16),
            pltpu.VMEM((2, 8, 8, 512), BF16),
            pltpu.VMEM((2, 8, 8, 512), BF16),
            pltpu.VMEM((2, 8, 128), BF16),
            pltpu.VMEM((2, 32, 8, 128), BF16),
            pltpu.VMEM((2, 32, 64, 128), BF16),
            pltpu.VMEM((2, 8, 4096), F32),
            pltpu.VMEM((2, 8, 4096), F32),
            pltpu.VMEM((2, 4096), F32),
            pltpu.VMEM((2, 2048), F32),
            pltpu.VMEM((2, 2048), F32),
            pltpu.VMEM((2, 2048), F32),
            pltpu.SemaphoreType.DMA((23,)),
            pltpu.SemaphoreType.DMA((2, 6)),
            pltpu.SemaphoreType.DMA((2, 6)),
        ],
        compiler_params=pltpu.CompilerParams(collective_id=0, has_side_effects=True),
    )(*args)
    return mixed.astype(BF16), new_state


def solution(mesh):
    weight = P(None, "tp", None, None)
    return jax.shard_map(
        on_device,
        mesh=mesh,
        in_specs=(
            P("tp", None, None),
            P(),
            weight,
            weight,
            weight,
            weight,
            weight,
            weight,
            P(),
            P(),
            P(),
            weight,
            weight,
        ),
        out_specs=(P("tp", None, None), weight),
        check_vma=False,
    )
```
